32 devices in a mesh: ep: 8 (over z, x), tp: 4 (over y, core).
Axes of the slice: x: 2, y: 2, z: 4, core: 2. Of those that a mesh axis runs over, the one named last changes fastest.
Arguments:
- tokens: bfloat16 [128, 1024], P('ep'), may hold values from -6 to 6
- memory: float32 [128, 4, 128, 256], P('ep', 'tp'), may hold values from -6 to 6
- log_scale: float32 [128, 4], P('ep', 'tp'), may hold values from -1 to 130
- mix_gain_in: float32 [1024], replicated, may hold values from 0.1 to 1.9
- w_query: bfloat16 [1024, 512], P(None, 'tp'), may hold values from -0.1875 to 0.1875
- w_key: bfloat16 [1024, 512], P(None, 'tp'), may hold values from -0.1875 to 0.1875
- w_value: bfloat16 [1024, 1024], P(None, 'tp'), may hold values from -0.1875 to 0.1875
- w_igate: bfloat16 [1024, 4], P(None, 'tp'), may hold values from -0.1875 to 0.1875
- w_fgate: bfloat16 [1024, 4], P(None, 'tp'), may hold values from -0.1875 to 0.1875
- igate_bias: float32 [4], P('tp'), may hold values from -1 to 1
- fgate_bias: float32 [4], P('tp'), may hold values from 0 to 4
- head_gain: float32 [1024], P('tp'), may hold values from 0.1 to 1.9
- w_output: bfloat16 [1024, 1024], P('tp'), may hold values from -0.1875 to 0.1875
- mix_gain_out: float32 [1024], replicated, may hold values from 0.1 to 1.9
- ffn_gain_in: float32 [1024], replicated, may hold values from 0.1 to 1.9
- routes: int32 [128, 6], P('ep'), may hold values from 0 to 7, all different within a row; in each aligned block of 16 rows (0 to 15, 16 to 31, ...) at most 16 rows name the same one
- route_weights: float32 [128, 6], P('ep'), may hold values from 0.1 to 1
- expert_gate: bfloat16 [8, 1024, 1024], P('ep', None, 'tp'), may hold values from -0.1875 to 0.1875
- expert_up: bfloat16 [8, 1024, 1024], P('ep', None, 'tp'), may hold values from -0.1875 to 0.1875
- expert_down: bfloat16 [8, 1024, 1024], P('ep', 'tp'), may hold values from -0.9375 to 0.9375
- ffn_gain_out: float32 [1024], P('tp'), may hold values from 0.1 to 1.9
Outputs:
- output: bfloat16 [128, 1024], P('ep', 'tp')
The draws below stay inside these ranges and needn't reach their ends.
Inputs may be any that keep to these rules, and one draw needn't show every extreme that they name: `routes`: among the 16 tokens of one index of ep no expert is named by more than 16 tokens, and in every draw some expert is named by exactly 16 of them.
All inputs are finite; a program needn't handle non-finite values.
Results may differ from the reference program's by a relative error of at most 0.02.
Values may be sent and summed in bfloat16 or wider, within the bound.
A program may use at most 64 MiB of HBM per device.

```python
import math
import jax
import jax.numpy as jnp
import numpy as np
from jax import lax

D = 1024
HEADS = 4
KEY_DIM = 128
VALUE_DIM = 256
EXPERT_WIDTH = 1024
TOP_K = 6
SEQ_G = 16
EXPERTS = 8
CAP = 16
BATCH = 128
N_EP = 8


def draw_log_scale(key, part):
    base_key = jax.random.fold_in(key, 11)
    values = jax.random.uniform(base_key, (BATCH, HEADS), jnp.float32, -1.0, 3.0)
    return values


def draw_expert_down(key, part):
    noise_key = jax.random.fold_in(key, 21)
    column_key = jax.random.fold_in(key, 22)
    raw = jnp.clip(jax.random.normal(noise_key, (EXPERTS, EXPERT_WIDTH, D), jnp.float32), -4.0, 4.0)
    spot = (jnp.arange(D, dtype=jnp.float32) + 0.5) / D
    jitter = jax.random.uniform(column_key, (D,), jnp.float32, -0.4, 0.4)
    ramp = 1.2 * (2.0 * spot - 1.0)
    scale = jnp.exp(ramp + jitter) * EXPERT_WIDTH ** (-0.5)
    return (raw * scale[None, None, :]).astype(jnp.bfloat16)


def block_scale(stream_key, dims, pieces, smallest, largest):
    loudness, own = 1.0, jax.random.fold_in(stream_key, 6)
    for dim, parts in pieces:
        heights = jnp.exp(jax.random.uniform(jax.random.fold_in(own, dim), (parts,), jnp.float32, smallest / len(pieces), largest / len(pieces)))
        loudness = loudness * jnp.repeat(heights, dims[dim] // parts).reshape([-1 if axis == dim else 1 for axis in range(len(dims))])
    return loudness


def assign_block(rng, own, number, rows, number_of, top, reach, lean):
    ranking = jax.random.permutation(rng, number_of)
    crowded, usual = portions_of(number_of, rows * top, reach, lean, True), portions_of(number_of, rows * top, reach, lean, False)
    places = jnp.arange(number_of)

    def named(sizes, turn):
        used = int((sizes > 0).sum())
        fixed = max(1, used // 4)
        moved = fixed + (places - fixed + turn * (used - fixed)) % max(1, number_of - fixed)
        return jnp.zeros((number_of,), jnp.int32).at[ranking[jnp.where(places < fixed, places, moved)]].set(jnp.asarray(sizes, jnp.int32))

    sizes = jnp.where(number % 4 == 0, named(crowded, number // 4), named(usual, number - number // 4 - 1))
    mixed = jax.random.permutation(jax.random.fold_in(own, 3), number_of)
    giver, taker = mixed[0:number_of // 2 * 2:2], mixed[1:number_of // 2 * 2:2]
    slack = jnp.minimum(sizes[giver] - 1, reach - sizes[taker]) // 2
    slack = jnp.where((giver == ranking[0]) | (taker == ranking[0]) | (sizes[taker] == 0), 0, jnp.maximum(slack, 0))
    moved = jax.random.randint(jax.random.fold_in(own, 4), (number_of // 2,), 0, 1 << 20) % (slack + 1)
    sizes = sizes.at[giver].add(-moved).at[taker].add(moved)
    members = jnp.searchsorted(jnp.cumsum(sizes), jnp.arange(rows * top), side="right").astype(jnp.int32)
    listing = members.reshape(top, rows).T
    listing = listing[jax.random.permutation(jax.random.fold_in(own, 1), rows)]
    turn = jax.random.randint(jax.random.fold_in(own, 2), (rows, 1), 0, top)
    return jnp.take_along_axis(listing, (jnp.arange(top)[None, :] + turn) % top, axis=1)


def portions_of(number_of, total, reach, lean, full):
    portions = [(1 << 20) // math.isqrt(rank ** lean) + 1 for rank in range(1, number_of + 1)]
    largest = reach if full else min(reach, max(-(-total // number_of), total * portions[0] // sum(portions)))
    least = 1 if total - largest >= number_of - 1 else 0
    counts, rest = [largest] + [least] * (number_of - 1), total - largest - least * (number_of - 1)
    while rest > 0:
        candidates = [i for i in range(1, number_of) if counts[i] < largest] or [i for i in range(1, number_of) if counts[i] < reach]
        pool, remaining = sum([portions[i] for i in candidates]), rest
        for i in candidates:
            addition = min(reach - counts[i], max(1, remaining * portions[i] // pool), rest)
            counts[i] = counts[i] + addition
            rest = rest - addition
    return np.array(counts)


def noise(key, shape, scale, bound, split=(), held_as=jnp.bfloat16):
    values = jax.random.normal(key, shape, jnp.float32) * scale
    if len(split) > 0:
        values = block_scale(key, shape, split, -0.22, 0.18) * values
    return jnp.clip(values, min=-bound, max=bound).astype(held_as)


def setup_inputs(seed: int = 0) -> dict:
    splits = jax.random.split(jax.random.key(seed), 22)
    tokens = noise(splits[0], (BATCH, D), 1.0, 6.0, ((0, 8),))
    memory = noise(splits[1], (BATCH, HEADS, KEY_DIM, VALUE_DIM), 1.0, 6.0, ((0, 8), (1, 4)), jnp.float32)
    log_scale = draw_log_scale(jax.random.fold_in(splits[21], 71), 0)
    mix_gain_in = jnp.clip(1.0 + 0.18 * jax.random.normal(splits[3], (D,), jnp.float32), 0.1, 1.9)
    w_query = noise(splits[4], (D, HEADS * KEY_DIM), D ** -0.5, 0.1875, ((1, 4),))
    w_key = noise(splits[5], (D, HEADS * KEY_DIM), D ** -0.5, 0.1875, ((1, 4),))
    w_value = noise(splits[6], (D, HEADS * VALUE_DIM), D ** -0.5, 0.1875, ((1, 4),))
    w_igate = noise(splits[7], (D, HEADS), D ** -0.5, 0.1875, ((1, 4),))
    w_fgate = noise(splits[8], (D, HEADS), D ** -0.5, 0.1875, ((1, 4),))
    igate_bias = jnp.clip(jax.random.uniform(splits[9], (HEADS,), jnp.float32, -1.0, 1.0) * block_scale(splits[9], (HEADS,), ((0, 4),), -0.4, 0.0), -1.0, 1.0)
    fgate_bias = jnp.clip(4.0 * jax.random.uniform(splits[10], (HEADS,), jnp.float32) ** block_scale(splits[10], (HEADS,), ((0, 4),), -0.2, 0.2), 0.0, 4.0)
    head_gain = jnp.clip(1.0 + 0.18 * jax.random.normal(splits[11], (HEADS * VALUE_DIM,), jnp.float32), 0.1, 1.9)
    w_output = noise(splits[12], (HEADS * VALUE_DIM, D), (HEADS * VALUE_DIM) ** -0.5, 0.1875, ((0, 4),))
    mix_gain_out = jnp.clip(1.0 + 0.18 * jax.random.normal(splits[13], (D,), jnp.float32), 0.1, 1.9)
    ffn_gain_in = jnp.clip(1.0 + 0.18 * jax.random.normal(splits[14], (D,), jnp.float32), 0.1, 1.9)
    routes_keys = jax.random.split(jax.random.fold_in(splits[15], 1), BATCH // SEQ_G)
    routes_turns = jax.random.permutation(jax.random.fold_in(splits[15], 3), BATCH // SEQ_G)
    routes = jax.vmap(lambda own, number: assign_block(jax.random.fold_in(splits[15], 2), own, number, SEQ_G, EXPERTS, TOP_K, CAP, 1))(routes_keys, routes_turns).reshape((BATCH, TOP_K))
    route_weights = jnp.clip(jnp.exp(math.log(1.0) - 2.3025851 * jax.random.uniform(splits[16], (BATCH, TOP_K), jnp.float32) ** block_scale(splits[16], (BATCH, TOP_K), ((0, 8),), -0.2, 0.2)), 0.1, 1.0)
    expert_gate = noise(splits[17], (EXPERTS, D, EXPERT_WIDTH), D ** -0.5, 0.1875, ((0, 8), (2, 4)))
    expert_up = noise(splits[18], (EXPERTS, D, EXPERT_WIDTH), D ** -0.5, 0.1875, ((0, 8), (2, 4)))
    expert_down = draw_expert_down(jax.random.fold_in(splits[21], 71), 0)
    ffn_gain_out = jnp.clip(1.0 + 0.18 * jax.random.normal(splits[20], (D,), jnp.float32), 0.1, 1.9)
    return dict(tokens=tokens, memory=memory, log_scale=log_scale, mix_gain_in=mix_gain_in, w_query=w_query, w_key=w_key, w_value=w_value, w_igate=w_igate, w_fgate=w_fgate, igate_bias=igate_bias, fgate_bias=fgate_bias, head_gain=head_gain, w_output=w_output, mix_gain_out=mix_gain_out, ffn_gain_in=ffn_gain_in, routes=routes, route_weights=route_weights, expert_gate=expert_gate, expert_up=expert_up, expert_down=expert_down, ffn_gain_out=ffn_gain_out)


EPS = 1e-06

def rms_scale(values):
    return lax.rsqrt(lax.optimization_barrier(jnp.mean(values * values, axis=-1, keepdims=True)) + EPS)

def reference(tokens, memory, log_scale, mix_gain_in, w_query, w_key, w_value, w_igate, w_fgate, igate_bias, fgate_bias, head_gain, w_output, mix_gain_out, ffn_gain_in, routes, route_weights, expert_gate, expert_up, expert_down, ffn_gain_out):
    f32 = jnp.float32
    bf16 = jnp.bfloat16
    xf = tokens.astype(f32)
    normed = (xf * rms_scale(xf) * mix_gain_in).astype(bf16)
    query = jnp.dot(normed, w_query, preferred_element_type=f32).reshape(BATCH, HEADS, KEY_DIM) * KEY_DIM ** (-0.5)
    keys = jnp.dot(normed, w_key, preferred_element_type=f32).reshape(BATCH, HEADS, KEY_DIM)
    values = jnp.dot(normed, w_value, preferred_element_type=f32).reshape(BATCH, HEADS, VALUE_DIM)
    in_pre = jnp.dot(normed, w_igate, preferred_element_type=f32) + igate_bias
    forget_log = jax.nn.log_sigmoid(jnp.dot(normed, w_fgate, preferred_element_type=f32) + fgate_bias)
    carried = forget_log + log_scale
    new_max = jnp.maximum(carried, in_pre)
    carry_weight = jnp.exp(carried - new_max)
    fresh_weight = jnp.exp(in_pre - new_max)
    recall = jnp.einsum('bhk,bhkv->bhv', query, memory, precision=lax.Precision.HIGHEST)
    match = lax.optimization_barrier(jnp.sum(query * keys, axis=-1))
    read = carry_weight[..., None] * recall + (fresh_weight * match)[..., None] * values
    headout = (read * rms_scale(read) * head_gain.reshape(HEADS, VALUE_DIM)).astype(bf16)
    per_head = jnp.einsum('bhv,hvd->bhd', headout.astype(f32), w_output.reshape(HEADS, VALUE_DIM, D).astype(f32)).astype(bf16)
    mixed = lax.optimization_barrier(jnp.sum(per_head.astype(f32), axis=1))
    resid = (xf + mixed * rms_scale(mixed) * mix_gain_out).astype(bf16)
    rf = resid.astype(f32)
    ffn_in = (rf * rms_scale(rf) * ffn_gain_in).astype(bf16)
    rows_total = BATCH * TOP_K
    limit = N_EP * CAP
    flat = routes.reshape(-1).astype(jnp.int32)

    def per_expert(done, expert):
        found = jnp.nonzero(flat == expert, size=limit, fill_value=rows_total)[0].astype(jnp.int32)
        token = jnp.minimum(found // TOP_K, BATCH - 1)
        picked = jnp.take(ffn_in, token, axis=0)
        gate = jnp.dot(picked, expert_gate[expert], preferred_element_type=f32)
        up = jnp.dot(picked, expert_up[expert], preferred_element_type=f32)
        act = (jax.nn.silu(gate) * up).astype(bf16)
        blocks = jnp.einsum('rtf,tfd->rtd', act.reshape(limit, HEADS, EXPERT_WIDTH // HEADS).astype(f32), expert_down[expert].reshape(HEADS, EXPERT_WIDTH // HEADS, D).astype(f32)).astype(bf16)
        result = lax.optimization_barrier(jnp.sum(blocks.astype(f32), axis=1)).astype(bf16)
        done = done.at[found].set(result, mode='drop')
        return (done, None)
    done, _ = lax.scan(per_expert, jnp.zeros((rows_total, D), bf16), jnp.arange(EXPERTS, dtype=jnp.int32))
    expert_rows = done.reshape(BATCH, TOP_K, D).astype(f32)
    routed = lax.optimization_barrier(jnp.sum(route_weights[..., None] * expert_rows, axis=1))
    return (rf + routed * rms_scale(routed) * ffn_gain_out).astype(bf16)
```

```python
import functools

import jax
import jax.numpy as jnp
from jax import lax
from jax.experimental import pallas as pl
from jax.experimental.pallas import tpu as pltpu
from jax.sharding import PartitionSpec as P

EPS = 1e-06


def rms_scale(values):
    return lax.rsqrt(jnp.mean(values * values, axis=-1, keepdims=True) + EPS)


def routed_device(
    tokens,
    memory,
    log_scale,
    mix_gain_in,
    w_query,
    w_key,
    w_value,
    w_igate,
    w_fgate,
    igate_bias,
    fgate_bias,
    head_gain,
    w_output,
    mix_gain_out,
    ffn_gain_in,
    routes,
    route_weights,
    expert_gate,
    expert_up,
    expert_down,
    ffn_gain_out,
):
    f32 = jnp.float32
    bf16 = jnp.bfloat16
    seqs, width = tokens.shape
    heads = log_scale.shape[1]
    key_dim = memory.shape[2]
    value_dim = memory.shape[3]
    xf = tokens.astype(f32)
    normed = (xf * rms_scale(xf) * mix_gain_in).astype(bf16)
    query = jnp.dot(normed, w_query, preferred_element_type=f32).reshape(
        seqs, heads, key_dim
    ) * key_dim ** (-0.5)
    keys = jnp.dot(normed, w_key, preferred_element_type=f32).reshape(seqs, heads, key_dim)
    values = jnp.dot(normed, w_value, preferred_element_type=f32).reshape(seqs, heads, value_dim)
    in_pre = jnp.dot(normed, w_igate, preferred_element_type=f32) + igate_bias
    forget_log = jax.nn.log_sigmoid(
        jnp.dot(normed, w_fgate, preferred_element_type=f32) + fgate_bias
    )
    carried = forget_log + log_scale
    new_max = jnp.maximum(carried, in_pre)
    carry_weight = jnp.exp(carried - new_max)
    fresh_weight = jnp.exp(in_pre - new_max)
    recall = jnp.einsum("shk,shkv->shv", query, memory, precision=lax.Precision.HIGHEST)
    match = jnp.sum(query * keys, axis=-1)
    read = carry_weight[..., None] * recall + (fresh_weight * match)[..., None] * values
    headout = (
        (read * rms_scale(read) * head_gain.reshape(heads, value_dim))
        .astype(bf16)
        .reshape(seqs, heads * value_dim)
    )
    partial_value = jnp.dot(headout, w_output, preferred_element_type=f32)
    mixed = lax.psum(partial_value.astype(jnp.bfloat16), "tp").astype(jnp.float32)
    resid = (xf + mixed * rms_scale(mixed) * mix_gain_out).astype(bf16)
    rf = resid.astype(f32)
    ffn_in = (rf * rms_scale(rf) * ffn_gain_in).astype(bf16)
    lanes = lax.axis_size("tp")
    quarter = width // lanes
    own = lax.axis_index("tp") * quarter
    local_experts = expert_gate.shape[0]
    experts_all = local_experts * lax.axis_size("ep")
    top = routes.shape[1]
    cap = min(seqs, max(2, 3 * seqs * top // (2 * experts_all)))
    flat = routes.reshape(-1)
    hits = (flat[:, None] == jnp.arange(experts_all, dtype=jnp.int32)[None, :]).astype(jnp.int32)
    earlier = jnp.cumsum(hits, axis=0) - hits
    slot = jnp.sum(earlier * hits, axis=1)
    place = (flat * cap + slot).reshape(seqs, top)
    picker = jnp.any(
        jnp.arange(experts_all * cap, dtype=jnp.int32)[:, None, None] == place[None, :, :], axis=2
    ).astype(bf16)
    outbound = (
        jnp.dot(picker, ffn_in, preferred_element_type=f32)
        .astype(bf16)
        .reshape(experts_all, cap, width)
    )
    arrived = lax.all_to_all(outbound, "ep", split_axis=0, concat_axis=0, tiled=True)
    items = arrived.shape[1]
    rows = arrived.reshape(-1, local_experts, items, width)
    gate = jnp.einsum("secd,edf->secf", rows, expert_gate, preferred_element_type=f32)
    up = jnp.einsum("secd,edf->secf", rows, expert_up, preferred_element_type=f32)
    act = (jax.nn.silu(gate) * up).astype(bf16)
    part = jnp.einsum("secf,efd->secd", act, expert_down, preferred_element_type=f32).reshape(
        -1, items, width
    )
    summed = lax.psum_scatter(
        part.astype(jnp.bfloat16), "tp", scatter_dimension=2, tiled=True
    ).astype(jnp.float32)
    done = summed.astype(bf16)
    returned = lax.all_to_all(done, "ep", split_axis=0, concat_axis=0, tiled=True)
    columns = returned.shape[2]
    chosen = jnp.take(returned.reshape(-1, columns), place.reshape(-1), axis=0).reshape(
        seqs, top, columns
    )
    routed = jnp.sum(route_weights[:, :, None] * chosen.astype(f32), axis=1)
    resid_part = lax.dynamic_slice_in_dim(rf, own, quarter, 1)
    total = lax.psum(jnp.sum(routed * routed, axis=1), "tp")
    scaled = routed * lax.rsqrt(total / width + EPS)[:, None]
    return (resid_part + scaled * ffn_gain_out).astype(bf16)


F32 = jnp.float32
BF16 = jnp.bfloat16
MESH = pl.DeviceIdType.MESH


def column_of(row):
    n = row.shape[1]
    eye = lax.broadcasted_iota(jnp.int32, (n, n), 0) == lax.broadcasted_iota(jnp.int32, (n, n), 1)
    return jnp.sum(jnp.where(eye, jnp.broadcast_to(row, (n, n)), 0.0), axis=1, keepdims=True)


def xor(a, b, size):
    total, bit = 0, 1
    while bit < size:
        total += bit * lax.rem(a // bit + b // bit, 2)
        bit *= 2
    return total


def arrived(ref, sem):
    pltpu.make_async_copy(ref, ref, sem).wait()


def layer_kernel(
    groups,
    lanes,
    tokens_hbm,
    memory_hbm,
    log_scale_hbm,
    gain_in_hbm,
    w_query_hbm,
    w_key_hbm,
    w_value_hbm,
    w_igate_hbm,
    w_fgate_hbm,
    igate_bias_hbm,
    fgate_bias_hbm,
    head_gain_hbm,
    w_output_hbm,
    gain_out_hbm,
    ffn_gain_hbm,
    routes_hbm,
    route_weights_hbm,
    gate_hbm,
    up_hbm,
    down_hbm,
    ffn_gain_out_hbm,
    out_ref,
    log_scale_ref,
    gain_in_ref,
    w_igate_ref,
    w_fgate_ref,
    igate_bias_ref,
    fgate_bias_ref,
    head_gain_ref,
    gain_out_ref,
    ffn_gain_ref,
    routes_ref,
    route_weights_ref,
    ffn_gain_out_ref,
    tokens_v,
    memory_v,
    w_qkv_v,
    w_output_v,
    gate_v,
    up_v,
    down_v,
    spread_v,
    recall_v,
    shares,
    rows,
    inbox,
    resid_v,
    parts,
    results,
    squares,
    load_sem,
    early_sem,
    late_sem,
    memory_sem,
    expert_sem,
    pair_send,
    pair_recv,
    entered,
    share_send,
    share_recv,
    rows_send,
    rows_recv,
    parts_send,
    parts_recv,
    squares_send,
    squares_recv,
):
    ep = lax.axis_index("ep")
    tp = lax.axis_index("tp")
    seqs, width = tokens_v.shape
    key_dim = memory_v.shape[1]
    value_dim = memory_v.shape[2]
    quarter = width // lanes
    core, chip = lax.rem(tp, 2), tp // 2
    slots, chips = groups // 2, lanes // 2
    depth, side = ep // 2, lax.rem(ep, 2)
    barrier = pltpu.get_barrier_semaphore()

    def lane_at(ahead, to_core):
        return 2 * lax.rem(chip + ahead, chips) + to_core

    pieces = memory_sem.shape[0]
    piece = seqs // pieces
    load_tokens = pltpu.make_async_copy(tokens_hbm, tokens_v, load_sem.at[0])
    load_gain = pltpu.make_async_copy(gain_in_hbm, gain_in_ref, load_sem.at[1])
    load_qkv = [
        pltpu.make_async_copy(src, w_qkv_v.at[:, pl.ds(at, src.shape[1])], load_sem.at[2])
        for src, at in (
            (w_query_hbm, 0),
            (w_key_hbm, key_dim),
            (w_value_hbm, 2 * key_dim),
        )
    ]
    load_output = pltpu.make_async_copy(w_output_hbm, w_output_v, load_sem.at[3])
    load_memory = [
        pltpu.make_async_copy(
            memory_hbm.at[pl.ds(i * piece, piece), 0],
            memory_v.at[pl.ds(i * piece, piece)],
            memory_sem.at[i],
        )
        for i in range(pieces)
    ]
    early = [
        pltpu.make_async_copy(src, dst, early_sem.at[i])
        for i, (src, dst) in enumerate(
            (
                (log_scale_hbm, log_scale_ref),
                (w_igate_hbm, w_igate_ref),
                (w_fgate_hbm, w_fgate_ref),
                (igate_bias_hbm, igate_bias_ref),
                (fgate_bias_hbm, fgate_bias_ref),
                (head_gain_hbm, head_gain_ref),
            )
        )
    ]
    late = [
        pltpu.make_async_copy(src, dst, late_sem.at[i])
        for i, (src, dst) in enumerate(
            (
                (gain_out_hbm, gain_out_ref),
                (ffn_gain_hbm, ffn_gain_ref),
                (routes_hbm, routes_ref),
                (route_weights_hbm, route_weights_ref),
                (ffn_gain_out_hbm, ffn_gain_out_ref),
            )
        )
    ]
    load_experts = [
        pltpu.make_async_copy(src.at[0], dst.at[0], expert_sem.at[i])
        for i, (src, dst) in enumerate(((gate_hbm, gate_v), (up_hbm, up_v), (down_hbm, down_v)))
    ]
    load_tokens.start()
    load_gain.start()
    for load in load_qkv:
        load.start()
    for load in load_memory:
        load.start()
    for load in early:
        load.start()
    load_output.start()

    def depth_of(slot):
        return slot - 1 + (slot - 1 + slots - depth) // slots

    def slot_of(group):
        return depth + (group // 2 - depth + slots - 1) // slots

    def greet(group, lane):
        pl.semaphore_signal(barrier, inc=1, device_id=(group, lane), device_id_type=MESH)

    for ahead in range(1, chips):
        greet(ep, lane_at(ahead, 0))
    for slot in range(1, slots):
        greet(xor(ep, 2 * slot + core, groups), 2 * chip + 1)

    @pl.when(core == 1)
    def _():
        greet(ep, tp - 1)
        greet(xor(ep, 1, groups), tp)

    for load in late:
        load.start()
    count = spread_v.shape[0]
    spread_v[...] = (
        lax.rem(lax.broadcasted_iota(jnp.int32, spread_v.shape, 0), seqs)
        == lax.broadcasted_iota(jnp.int32, spread_v.shape, 1) // key_dim
    ).astype(F32).astype(BF16)

    load_tokens.wait()
    load_gain.wait()
    xf = tokens_v[...].astype(F32)
    normed = (xf * rms_scale(xf) * gain_in_ref[...]).astype(BF16)
    arrived(w_qkv_v, load_sem.at[2])
    qkv = jnp.dot(normed, w_qkv_v[...], preferred_element_type=F32)
    query = qkv[:, :key_dim] * key_dim ** (-0.5)
    keys = qkv[:, key_dim : 2 * key_dim]
    values = qkv[:, 2 * key_dim :]
    for load in load_experts:
        load.start()
    for load in early:
        load.wait()
    nf = normed.astype(F32)
    in_pre = (
        jnp.sum(nf * w_igate_ref[...].astype(F32), axis=1, keepdims=True) + igate_bias_ref[...]
    )
    fpre = jnp.sum(nf * w_fgate_ref[...].astype(F32), axis=1, keepdims=True) + fgate_bias_ref[...]
    forget_log = jnp.minimum(fpre, 0.0) - jnp.log1p(jnp.exp(-jnp.abs(fpre)))
    carried = forget_log + column_of(log_scale_ref[...])
    new_max = jnp.maximum(carried, in_pre)
    carry_weight = jnp.exp(carried - new_max)
    fresh_weight = jnp.exp(in_pre - new_max)
    match = jnp.sum(query * keys, axis=1, keepdims=True)
    high = query.astype(BF16).astype(F32)
    middle = (query - high).astype(BF16).astype(F32)
    low = query - high - middle
    turned = jnp.concatenate([high, middle, low], axis=0).T.astype(BF16)

    @pl.when(core == 0)
    def _():
        pl.semaphore_wait(barrier, lanes - 1)
        pl.semaphore_signal(entered, inc=1, device_id=(ep, tp + 1), device_id_type=MESH)

    for i in range(pieces):
        load_memory[i].wait()
        wide = jnp.dot(
            turned,
            spread_v[:, i * piece * key_dim : (i + 1) * piece * key_dim],
            preferred_element_type=F32,
        )
        for j in range(piece):
            s = i * piece + j
            column = wide[:, j * key_dim : (j + 1) * key_dim]
            for at in range(0, value_dim, key_dim):
                recall_v[s : s + 1, at : at + key_dim] = jnp.sum(
                    column * memory_v[s, :, at : at + key_dim], axis=0, keepdims=True
                )
    read = carry_weight * recall_v[...] + (fresh_weight * match) * values
    headout = (read * rms_scale(read) * head_gain_ref[...]).astype(BF16)
    load_output.wait()
    shares[0] = jnp.dot(headout, w_output_v[...], preferred_element_type=F32).astype(BF16)

    @pl.when(core == 1)
    def _():
        pl.semaphore_wait(entered, 1)


    def share(ahead, to_core):
        pltpu.make_async_remote_copy(
            src_ref=shares.at[0],
            dst_ref=shares.at[2 * ahead + lax.rem(core + to_core, 2)],
            send_sem=share_send,
            recv_sem=share_recv,
            device_id=(ep, lane_at(ahead, to_core)),
            device_id_type=MESH,
        ).start()

    for ahead in range(1, chips):
        share(ahead, 1)
    share(0, 1 - core)
    for ahead in range(1, chips):
        share(ahead, 0)
    pairs = []
    for i, ref in enumerate((gate_v, up_v, down_v)):
        load_experts[i].wait()
        copy = pltpu.make_async_remote_copy(
            src_ref=ref.at[0],
            dst_ref=ref.at[1],
            send_sem=pair_send.at[i],
            recv_sem=pair_recv.at[i],
            device_id=(ep, tp + 1 - 2 * core),
            device_id_type=MESH,
        )
        copy.start()
        pairs.append(copy)
    for load in late:
        load.wait()
    mine = [
        column_of(
            jnp.sum(
                jnp.where(routes_ref[...] == xor(ep, off, groups), route_weights_ref[...], 0.0),
                axis=0,
                keepdims=True,
            )
        )
        for off in range(groups)
    ]
    arrived(shares.at[pl.ds(1, lanes - 1)], share_recv)
    mixed = shares[0].astype(F32)
    for other in range(1, lanes):
        mixed = mixed + shares[other].astype(F32)
    resid = (xf + mixed * rms_scale(mixed) * gain_out_ref[...]).astype(BF16)
    rf = resid.astype(F32)
    ffn_in = (rf * rms_scale(rf) * ffn_gain_ref[...]).astype(BF16)
    rows[...] = ffn_in

    @pl.when(core == 1)
    def _():
        pl.semaphore_wait(barrier, groups - 1)
        for off in range(groups - 1, 0, -1):
            group = xor(ep, off, groups)
            pltpu.make_async_remote_copy(
                src_ref=rows,
                dst_ref=inbox.at[slot_of(group)] if off > 1 else inbox.at[0],
                send_sem=rows_send,
                recv_sem=rows_recv.at[slot_of(group)] if off > 1 else rows_recv.at[0],
                device_id=(group, 2 * chip + off % 2),
                device_id_type=MESH,
            ).start()

    for q in range(lanes):
        resid_v[q] = rf[:, q * quarter : (q + 1) * quarter]

    @pl.when(core == 0)
    def _():
        inbox[0] = rows[...]

    @pl.when(core == 1)
    def _():
        arrived(inbox.at[0], rows_recv.at[0])

    for copy in pairs:
        copy.wait_recv()

    def result(slot, ahead, to_core):
        off = core if slot == 0 else 2 * xor(depth, depth_of(slot), slots) + core
        dst = results.at[off * chips + ahead]
        return pltpu.make_async_remote_copy(
            src_ref=parts.at[slot, lane_at(ahead, to_core)],
            dst_ref=dst,
            send_sem=parts_send.at[min(slot, 1)],
            recv_sem=parts_recv.at[0],
            device_id=(xor(ep, off, groups), lane_at(ahead, to_core)),
            device_id_type=MESH,
        )

    for slot in range(slots):
        if slot:
            arrived(inbox.at[slot], rows_recv.at[slot])
        x = inbox[slot]
        act = [
            (
                jax.nn.silu(jnp.dot(x, gate_v[block], preferred_element_type=F32))
                * jnp.dot(x, up_v[block], preferred_element_type=F32)
            ).astype(BF16)
            for block in range(2)
        ]
        for q in range(lanes):
            parts[slot, q] = sum(
                jnp.dot(
                    act[block],
                    down_v[block, :, q * quarter : (q + 1) * quarter],
                    preferred_element_type=F32,
                )
                for block in range(2)
            ).astype(BF16)
        for ahead in range(chips - 1, 0, -1):
            for to_core in range(2):
                result(slot, ahead, to_core).start()
        if slot:
            for to_core in range(2):
                result(slot, 0, to_core).start()
        else:

            @pl.when(core == 1)
            def _():
                for to_core in range(2):
                    result(0, 0, to_core).start()

            @pl.when(core == 0)
            def _():
                pltpu.make_async_remote_copy(
                    src_ref=parts.at[0, tp + 1],
                    dst_ref=results.at[0],
                    send_sem=parts_send.at[0],
                    recv_sem=parts_recv.at[1],
                    device_id=(ep, tp + 1),
                    device_id_type=MESH,
                ).start()
                results[0] = parts[0, tp]

    arrived(results.at[pl.ds(1, groups * chips - 1)], parts_recv.at[0])

    @pl.when(core == 1)
    def _():
        arrived(results.at[0], parts_recv.at[1])

    routed = None
    for off in range(groups):
        total = None
        for ahead in range(chips):
            part = results[off * chips + ahead].astype(F32)
            total = part if total is None else total + part
        term = mine[off] * total.astype(BF16).astype(F32)
        routed = term if routed is None else routed + term
    wide = squares.shape[2]
    eye = lax.broadcasted_iota(jnp.int32, (seqs, wide), 0) == lax.broadcasted_iota(
        jnp.int32, (seqs, wide), 1
    )
    squares[0] = jnp.sum(
        jnp.where(eye, jnp.sum(routed * routed, axis=1, keepdims=True), 0.0),
        axis=0,
        keepdims=True,
    )
    for ahead in range(chips - 1, -1, -1):
        for flip in range(2):
            if ahead or flip:
                pltpu.make_async_remote_copy(
                    src_ref=squares.at[0],
                    dst_ref=squares.at[2 * ahead + flip],
                    send_sem=squares_send,
                    recv_sem=squares_recv,
                    device_id=(ep, lane_at(ahead, lax.rem(core + flip, 2))),
                    device_id_type=MESH,
                ).start()
    arrived(shares.at[pl.ds(1, lanes - 1)], share_send)
    for copy in pairs:
        copy.wait_send()
    arrived(parts.at[pl.ds(1, slots - 1)], parts_send.at[1])

    @pl.when(core == 0)
    def _():
        arrived(parts.at[0, pl.ds(1, lanes - 1)], parts_send.at[0])

    @pl.when(core == 1)
    def _():
        arrived(parts.at[0], parts_send.at[0])
        hidden = gate_v.shape[2]
        arrived(gate_v.at[0, pl.ds(0, (groups - 1) * seqs * width // hidden)], rows_send)

    arrived(squares.at[pl.ds(1, lanes - 1)], squares_recv)
    total = squares[0]
    for other in range(1, lanes):
        total = total + squares[other]
    scale = jnp.sum(
        jnp.where(eye, lax.rsqrt(total / width + EPS), 0.0), axis=1, keepdims=True
    )
    scaled = routed * scale
    out_ref[...] = (resid_v[tp] + scaled * ffn_gain_out_ref[...]).astype(BF16)
    arrived(squares.at[pl.ds(1, lanes - 1)], squares_send)


def per_device(*args):
    (
        tokens,
        memory,
        log_scale,
        mix_gain_in,
        w_query,
        w_key,
        w_value,
        w_igate,
        w_fgate,
        igate_bias,
        fgate_bias,
        head_gain,
        w_output,
        mix_gain_out,
        ffn_gain_in,
        routes,
        route_weights,
        expert_gate,
        expert_up,
        expert_down,
        ffn_gain_out,
    ) = args
    groups = lax.axis_size("ep")
    lanes = lax.axis_size("tp")
    seqs, width = tokens.shape
    local_experts, _, hidden = expert_gate.shape
    top = routes.shape[1]
    if (
        local_experts != 1
        or log_scale.shape[1] != 1
        or 2 * top < groups
        or groups & (groups - 1)
        or groups < 4
        or lanes % 2
        or lanes < 4
        or memory.shape[3] % memory.shape[2]
        or (groups - 1) * seqs > hidden
        or width % hidden
    ):
        return routed_device(*args)
    quarter = width // lanes
    key_dim, value_dim = memory.shape[2:]
    vmem = pl.BlockSpec(memory_space=pltpu.VMEM)
    hbm = pl.BlockSpec(memory_space=pl.ANY)
    dma = pltpu.SemaphoreType.DMA
    pieces = 4 if seqs % 4 == 0 else 1
    operands = (
        tokens,
        memory,
        log_scale.T,
        mix_gain_in.reshape(1, -1),
        w_query,
        w_key,
        w_value,
        w_igate.T,
        w_fgate.T,
        igate_bias.reshape(1, 1),
        fgate_bias.reshape(1, 1),
        head_gain.reshape(1, -1),
        w_output,
        mix_gain_out.reshape(1, -1),
        ffn_gain_in.reshape(1, -1),
        routes.T,
        route_weights.T,
        expert_gate,
        expert_up,
        expert_down,
        ffn_gain_out.reshape(1, -1),
    )
    held = (2, 3, 7, 8, 9, 10, 11, 13, 14, 15, 16, 20)
    return pl.pallas_call(
        functools.partial(layer_kernel, groups, lanes),
        out_shape=pltpu.VMEM((seqs, quarter), BF16),
        in_specs=[hbm for _ in operands],
        out_specs=vmem,
        scratch_shapes=[
            *[pltpu.VMEM(operands[i].shape, operands[i].dtype) for i in held],
            pltpu.VMEM((seqs, width), BF16),
            pltpu.VMEM((seqs, key_dim, value_dim), F32),
            pltpu.VMEM((width, 2 * key_dim + value_dim), BF16),
            pltpu.VMEM(w_output.shape, BF16),
            pltpu.VMEM((2, width, hidden), BF16),
            pltpu.VMEM((2, width, hidden), BF16),
            pltpu.VMEM((2, hidden, width), BF16),
            pltpu.VMEM((3 * seqs, seqs * key_dim), BF16),
            pltpu.VMEM((seqs, value_dim), F32),
            pltpu.VMEM((lanes, seqs, width), BF16),
            pltpu.VMEM((seqs, width), BF16),
            pltpu.VMEM((groups // 2, seqs, width), BF16),
            pltpu.VMEM((lanes, seqs, quarter), F32),
            pltpu.VMEM((groups // 2, lanes, seqs, quarter), BF16),
            pltpu.VMEM((groups * lanes // 2, seqs, quarter), BF16),
            pltpu.VMEM((lanes, 1, 128), F32),
            dma((4,)),
            dma((6,)),
            dma((5,)),
            dma((pieces,)),
            dma((3,)),
            dma((3,)),
            dma((3,)),
            pltpu.SemaphoreType.REGULAR,
            dma(()),
            dma(()),
            dma(()),
            dma((groups // 2,)),
            dma((2,)),
            dma((2,)),
            dma(()),
            dma(()),
        ],
        compiler_params=pltpu.CompilerParams(
            collective_id=0,
            has_side_effects=True,
            vmem_limit_bytes=59 * 1024 * 1024,
        ),
        name="layer",
    )(*operands)


def solution(mesh):
    return jax.shard_map(
        per_device,
        mesh=mesh,
        in_specs=(
            P("ep", None),
            P("ep", "tp", None, None),
            P("ep", "tp"),
            P(),
            P(None, "tp"),
            P(None, "tp"),
            P(None, "tp"),
            P(None, "tp"),
            P(None, "tp"),
            P("tp"),
            P("tp"),
            P("tp"),
            P("tp", None),
            P(),
            P(),
            P("ep", None),
            P("ep", None),
            P("ep", None, "tp"),
            P("ep", None, "tp"),
            P("ep", "tp", None),
            P("tp"),
        ),
        out_specs=P("ep", "tp"),
        check_vma=False,
    )
```

```python
import functools

import jax
import jax.numpy as jnp
from jax import lax
from jax.experimental import pallas as pl
from jax.experimental.pallas import tpu as pltpu
from jax.sharding import PartitionSpec as P

EPS = 1e-06


def rms_scale(values):
    return lax.rsqrt(jnp.mean(values * values, axis=-1, keepdims=True) + EPS)


def routed_device(
    tokens,
    memory,
    log_scale,
    mix_gain_in,
    w_query,
    w_key,
    w_value,
    w_igate,
    w_fgate,
    igate_bias,
    fgate_bias,
    head_gain,
    w_output,
    mix_gain_out,
    ffn_gain_in,
    routes,
    route_weights,
    expert_gate,
    expert_up,
    expert_down,
    ffn_gain_out,
):
    f32 = jnp.float32
    bf16 = jnp.bfloat16
    seqs, width = tokens.shape
    heads = log_scale.shape[1]
    key_dim = memory.shape[2]
    value_dim = memory.shape[3]
    xf = tokens.astype(f32)
    normed = (xf * rms_scale(xf) * mix_gain_in).astype(bf16)
    query = jnp.dot(normed, w_query, preferred_element_type=f32).reshape(
        seqs, heads, key_dim
    ) * key_dim ** (-0.5)
    keys = jnp.dot(normed, w_key, preferred_element_type=f32).reshape(seqs, heads, key_dim)
    values = jnp.dot(normed, w_value, preferred_element_type=f32).reshape(seqs, heads, value_dim)
    in_pre = jnp.dot(normed, w_igate, preferred_element_type=f32) + igate_bias
    forget_log = jax.nn.log_sigmoid(
        jnp.dot(normed, w_fgate, preferred_element_type=f32) + fgate_bias
    )
    carried = forget_log + log_scale
    new_max = jnp.maximum(carried, in_pre)
    carry_weight = jnp.exp(carried - new_max)
    fresh_weight = jnp.exp(in_pre - new_max)
    recall = jnp.einsum("shk,shkv->shv", query, memory, precision=lax.Precision.HIGHEST)
    match = jnp.sum(query * keys, axis=-1)
    read = carry_weight[..., None] * recall + (fresh_weight * match)[..., None] * values
    headout = (
        (read * rms_scale(read) * head_gain.reshape(heads, value_dim))
        .astype(bf16)
        .reshape(seqs, heads * value_dim)
    )
    partial_value = jnp.dot(headout, w_output, preferred_element_type=f32)
    mixed = lax.psum(partial_value.astype(jnp.bfloat16), "tp").astype(jnp.float32)
    resid = (xf + mixed * rms_scale(mixed) * mix_gain_out).astype(bf16)
    rf = resid.astype(f32)
    ffn_in = (rf * rms_scale(rf) * ffn_gain_in).astype(bf16)
    lanes = lax.axis_size("tp")
    quarter = width // lanes
    own = lax.axis_index("tp") * quarter
    local_experts = expert_gate.shape[0]
    experts_all = local_experts * lax.axis_size("ep")
    top = routes.shape[1]
    cap = min(seqs, max(2, 3 * seqs * top // (2 * experts_all)))
    flat = routes.reshape(-1)
    hits = (flat[:, None] == jnp.arange(experts_all, dtype=jnp.int32)[None, :]).astype(jnp.int32)
    earlier = jnp.cumsum(hits, axis=0) - hits
    slot = jnp.sum(earlier * hits, axis=1)
    place = (flat * cap + slot).reshape(seqs, top)
    picker = jnp.any(
        jnp.arange(experts_all * cap, dtype=jnp.int32)[:, None, None] == place[None, :, :], axis=2
    ).astype(bf16)
    outbound = (
        jnp.dot(picker, ffn_in, preferred_element_type=f32)
        .astype(bf16)
        .reshape(experts_all, cap, width)
    )
    arrived = lax.all_to_all(outbound, "ep", split_axis=0, concat_axis=0, tiled=True)
    items = arrived.shape[1]
    rows = arrived.reshape(-1, local_experts, items, width)
    gate = jnp.einsum("secd,edf->secf", rows, expert_gate, preferred_element_type=f32)
    up = jnp.einsum("secd,edf->secf", rows, expert_up, preferred_element_type=f32)
    act = (jax.nn.silu(gate) * up).astype(bf16)
    part = jnp.einsum("secf,efd->secd", act, expert_down, preferred_element_type=f32).reshape(
        -1, items, width
    )
    summed = lax.psum_scatter(
        part.astype(jnp.bfloat16), "tp", scatter_dimension=2, tiled=True
    ).astype(jnp.float32)
    done = summed.astype(bf16)
    returned = lax.all_to_all(done, "ep", split_axis=0, concat_axis=0, tiled=True)
    columns = returned.shape[2]
    chosen = jnp.take(returned.reshape(-1, columns), place.reshape(-1), axis=0).reshape(
        seqs, top, columns
    )
    routed = jnp.sum(route_weights[:, :, None] * chosen.astype(f32), axis=1)
    resid_part = lax.dynamic_slice_in_dim(rf, own, quarter, 1)
    total = lax.psum(jnp.sum(routed * routed, axis=1), "tp")
    scaled = routed * lax.rsqrt(total / width + EPS)[:, None]
    return (resid_part + scaled * ffn_gain_out).astype(bf16)


F32 = jnp.float32
BF16 = jnp.bfloat16
MESH = pl.DeviceIdType.MESH


def column_of(row):
    n = row.shape[1]
    eye = lax.broadcasted_iota(jnp.int32, (n, n), 0) == lax.broadcasted_iota(jnp.int32, (n, n), 1)
    return jnp.sum(jnp.where(eye, jnp.broadcast_to(row, (n, n)), 0.0), axis=1, keepdims=True)


def xor(a, b, size):
    total, bit = 0, 1
    while bit < size:
        total += bit * lax.rem(a // bit + b // bit, 2)
        bit *= 2
    return total


def arrived(ref, sem):
    pltpu.make_async_copy(ref, ref, sem).wait()


def layer_kernel(
    groups,
    lanes,
    tokens_hbm,
    memory_hbm,
    log_scale_hbm,
    gain_in_hbm,
    w_query_hbm,
    w_key_hbm,
    w_value_hbm,
    w_igate_hbm,
    w_fgate_hbm,
    igate_bias_hbm,
    fgate_bias_hbm,
    head_gain_hbm,
    w_output_hbm,
    gain_out_hbm,
    ffn_gain_hbm,
    routes_hbm,
    route_weights_hbm,
    gate_hbm,
    up_hbm,
    down_hbm,
    ffn_gain_out_hbm,
    out_ref,
    log_scale_ref,
    gain_in_ref,
    routes_ref,
    route_weights_ref,
    w_gates_v,
    biases_v,
    gains_v,
    heads_v,
    tokens_v,
    memory_v,
    w_qkv_v,
    w_output_v,
    into_v,
    down_v,
    spread_v,
    wide_v,
    recall_v,
    shares,
    rows,
    inbox,
    resid_v,
    parts,
    results,
    routed_v,
    squares,
    load_sem,
    early_sem,
    late_sem,
    expert_sem,
    pair_send,
    pair_recv,
    entered,
    share_send,
    share_recv,
    rows_send,
    rows_recv,
    resid_sem,
    parts_send,
    parts_recv,
    routed_sem,
    squares_sem,
):
    ep = lax.axis_index("ep")
    tp = lax.axis_index("tp")
    seqs, width = tokens_v.shape
    key_dim = memory_v.shape[1]
    value_dim = memory_v.shape[2]
    quarter, half = width // lanes, 2 * width // lanes
    core, chip = lax.rem(tp, 2), tp // 2
    slots, chips = groups // 2, lanes // 2
    depth, side = ep // 2, lax.rem(ep, 2)
    barrier = pltpu.get_barrier_semaphore()

    def lane_at(ahead, to_core):
        return 2 * lax.rem(chip + ahead, chips) + to_core

    load_tokens = pltpu.make_async_copy(tokens_hbm, tokens_v, load_sem.at[0])
    load_gain = pltpu.make_async_copy(gain_in_hbm, gain_in_ref, load_sem.at[1])
    load_qkv = [
        pltpu.make_async_copy(src, w_qkv_v.at[:, pl.ds(at, src.shape[1])], load_sem.at[2])
        for src, at in (
            (w_query_hbm, 0),
            (w_key_hbm, key_dim),
            (w_value_hbm, 2 * key_dim),
        )
    ]
    load_output = pltpu.make_async_copy(w_output_hbm, w_output_v, load_sem.at[3])
    load_memory = pltpu.make_async_copy(memory_hbm.at[:, 0], memory_v, load_sem.at[4])

    def loads(sems, *copies):
        return [pltpu.make_async_copy(src, dst, sems.at[i]) for src, dst, i in copies]

    early = loads(
        early_sem,
        (w_igate_hbm, w_gates_v.at[0], 0),
        (w_fgate_hbm, w_gates_v.at[1], 0),
        (log_scale_hbm, log_scale_ref, 1),
        (igate_bias_hbm, biases_v.at[0], 2),
        (fgate_bias_hbm, biases_v.at[1], 2),
    )
    late = loads(
        late_sem,
        (head_gain_hbm, heads_v.at[0], 0),
        (ffn_gain_out_hbm, heads_v.at[1], 0),
        (gain_out_hbm, gains_v.at[0], 1),
        (ffn_gain_hbm, gains_v.at[1], 1),
        (routes_hbm, routes_ref, 2),
        (route_weights_hbm, route_weights_ref, 3),
    )
    experts = loads(
        expert_sem,
        (gate_hbm.at[0], into_v.at[0, 0], 0),
        (up_hbm.at[0], into_v.at[0, 1], 0),
        (down_hbm.at[0], down_v.at[0], 1),
    )
    load_tokens.start()
    load_gain.start()
    for load in early:
        load.start()
    for load in load_qkv:
        load.start()

    def depth_of(slot):
        return slot - 1 + (slot - 1 + slots - depth) // slots

    def greet(group, lane):
        pl.semaphore_signal(barrier, inc=1, device_id=(group, lane), device_id_type=MESH)

    for slot in range(1, slots):
        greet(xor(ep, 2 * slot + core, groups), 2 * chip + 1)

    @pl.when(core == 1)
    def _():
        for ahead in range(chips):
            greet(ep, lane_at(ahead, 0))
        greet(xor(ep, 1, groups), tp)

    spread_v[...] = (
        lax.rem(lax.broadcasted_iota(jnp.int32, spread_v.shape, 0), seqs)
        == lax.broadcasted_iota(jnp.int32, spread_v.shape, 1) // key_dim
    ).astype(F32).astype(BF16)

    load_memory.start()
    load_output.start()
    for load in late:
        load.start()
    load_tokens.wait()
    load_gain.wait()
    xf = tokens_v[...].astype(F32)
    normed = (xf * rms_scale(xf) * gain_in_ref[...]).astype(BF16)
    arrived(w_gates_v, early_sem.at[0])
    arrived(log_scale_ref, early_sem.at[1])
    arrived(biases_v, early_sem.at[2])
    nf = normed.astype(F32)
    in_pre = jnp.sum(nf * w_gates_v[0].astype(F32), axis=1, keepdims=True) + biases_v[0]
    fpre = jnp.sum(nf * w_gates_v[1].astype(F32), axis=1, keepdims=True) + biases_v[1]
    forget_log = jnp.minimum(fpre, 0.0) - jnp.log1p(jnp.exp(-jnp.abs(fpre)))
    carried = forget_log + column_of(log_scale_ref[...])
    new_max = jnp.maximum(carried, in_pre)
    carry_weight = jnp.exp(carried - new_max)
    fresh_weight = jnp.exp(in_pre - new_max)
    arrived(w_qkv_v, load_sem.at[2])

    @pl.when(core == 0)
    def _():
        pl.semaphore_wait(barrier, chips)
        pl.semaphore_signal(entered, inc=1, device_id=(ep, tp + 1), device_id_type=MESH)

    qkv = jnp.dot(normed, w_qkv_v[...], preferred_element_type=F32)
    query = qkv[:, :key_dim] * key_dim ** (-0.5)
    keys = qkv[:, key_dim : 2 * key_dim]
    values = qkv[:, 2 * key_dim :]
    high = query.astype(BF16).astype(F32)
    middle = (query - high).astype(BF16).astype(F32)
    low = query - high - middle
    turned = jnp.concatenate([high, middle, low], axis=0).T.astype(BF16)
    wide_v[...] = jnp.dot(turned, spread_v[...], preferred_element_type=F32)
    match = jnp.sum(query * keys, axis=1, keepdims=True)
    fresh = (fresh_weight * match) * values
    load_memory.wait()
    load_output.wait()
    arrived(heads_v, late_sem.at[0])
    for load in experts:
        load.start()
    for s in range(seqs):
        column = wide_v[:, s * key_dim : (s + 1) * key_dim]
        for at in range(0, value_dim, key_dim):
            recall_v[s : s + 1, at : at + key_dim] = jnp.sum(
                column * memory_v[s, :, at : at + key_dim], axis=0, keepdims=True
            )
    read = carry_weight * recall_v[...] + fresh
    headout = (read * heads_v[0]).astype(BF16)
    shares[0] = (
        jnp.dot(headout, w_output_v[...], preferred_element_type=F32) * rms_scale(read)
    ).astype(BF16)

    @pl.when(core == 1)
    def _():
        pl.semaphore_wait(entered, 1)


    def share(ahead):
        pltpu.make_async_remote_copy(
            src_ref=shares.at[0],
            dst_ref=shares.at[2 * ahead + 1 - core],
            send_sem=share_send,
            recv_sem=share_recv,
            device_id=(ep, lane_at(ahead, 1)),
            device_id_type=MESH,
        ).start()

    for ahead in range(1, chips):
        share(ahead)

    @pl.when(core == 0)
    def _():
        share(0)

    pairs = []
    for i, ref in enumerate((into_v, down_v)):
        arrived(ref.at[0], expert_sem.at[i])
        copy = pltpu.make_async_remote_copy(
            src_ref=ref.at[0],
            dst_ref=ref.at[1],
            send_sem=pair_send.at[i],
            recv_sem=pair_recv.at[i],
            device_id=(ep, tp + 1 - 2 * core),
            device_id_type=MESH,
        )
        copy.start()
        pairs.append(copy)
    arrived(gains_v, late_sem.at[1])
    arrived(routes_ref, late_sem.at[2])
    arrived(route_weights_ref, late_sem.at[3])
    mine = [
        column_of(
            jnp.sum(
                jnp.where(routes_ref[...] == xor(ep, off, groups), route_weights_ref[...], 0.0),
                axis=0,
                keepdims=True,
            )
        )
        for off in range(groups)
    ]

    def send_rows(group, slot, to_core):
        pltpu.make_async_remote_copy(
            src_ref=rows,
            dst_ref=inbox.at[slot],
            send_sem=rows_send,
            recv_sem=rows_recv.at[slot],
            device_id=(group, 2 * chip + to_core),
            device_id_type=MESH,
        ).start()

    @pl.when(core == 1)
    def _():
        arrived(shares.at[pl.ds(1, lanes - 1)], share_recv)
        mixed = shares[0].astype(F32)
        for other in range(1, lanes):
            mixed = mixed + shares[other].astype(F32)
        resid = (xf + mixed * rms_scale(mixed) * gains_v[0]).astype(BF16)
        rf = resid.astype(F32)
        rows[...] = (rf * rms_scale(rf) * gains_v[1]).astype(BF16)
        pl.semaphore_wait(barrier, groups - 1)
        upper = depth // (slots // 2)
        level = upper * depth + (1 - upper) * (slots - 1 - depth)
        for i in range(slots - 1):
            step = i + (i - level + slots) // slots
            to = upper * step + (1 - upper) * (slots - 1 - step)
            slot = depth + (to - depth + slots - 1) // slots
            for to_core in (1, 0):
                send_rows(2 * to + lax.rem(side + to_core, 2), slot - to_core * (1 // slot), to_core)
        send_rows(xor(ep, 1, groups), 1, 1)
        send_rows(ep, 0, 0)
        for q in range(lanes):
            resid_v[q] = resid[:, q * quarter : (q + 1) * quarter]
        pltpu.make_async_remote_copy(
            src_ref=resid_v.at[tp - 1],
            dst_ref=resid_v.at[tp - 1],
            send_sem=resid_sem.at[0],
            recv_sem=resid_sem.at[1],
            device_id=(ep, tp - 1),
            device_id_type=MESH,
        ).start()

    for copy in pairs:
        copy.wait_recv()

    nearest = depth_of(1)

    def result(slot, ahead):
        level = depth_of(slot)
        if slot < 2:
            turn = core if slot == 0 else 1 - core
            level = turn * nearest + (1 - turn) * depth
        off = 2 * xor(depth, level, slots) + core
        return pltpu.make_async_remote_copy(
            src_ref=parts.at[slot, lax.rem(chip + ahead, chips)],
            dst_ref=results.at[off * chips + ahead],
            send_sem=parts_send,
            recv_sem=parts_recv,
            device_id=(xor(ep, off, groups), lane_at(ahead, 1)),
            device_id_type=MESH,
        )

    for slot in range(slots):
        arrived(inbox.at[slot], rows_recv.at[slot])
        x = inbox[slot]
        act = [
            (
                jax.nn.silu(jnp.dot(x, into_v[block, 0], preferred_element_type=F32))
                * jnp.dot(x, into_v[block, 1], preferred_element_type=F32)
            ).astype(BF16)
            for block in range(2)
        ]
        for y in range(chips):
            parts[slot, y] = sum(
                jnp.dot(
                    act[block],
                    down_v[block, :, y * half : (y + 1) * half],
                    preferred_element_type=F32,
                )
                for block in range(2)
            ).astype(BF16)
        for ahead in range(chips - 1, -1, -1):
            result(slot, ahead).start()

    wide = squares.shape[2]
    eye = lax.broadcasted_iota(jnp.int32, (seqs, wide), 0) == lax.broadcasted_iota(
        jnp.int32, (seqs, wide), 1
    )

    def send(ref, at, sems, lane):
        pltpu.make_async_remote_copy(
            src_ref=ref.at[0],
            dst_ref=ref.at[at],
            send_sem=sems.at[0],
            recv_sem=sems.at[1],
            device_id=(ep, lane),
            device_id_type=MESH,
        ).start()

    @pl.when(core == 1)
    def _():
        arrived(results, parts_recv)
        routed = None
        for off in range(groups):
            total = None
            for ahead in range(chips):
                part = results[off * chips + ahead].astype(F32)
                total = part if total is None else total + part
            term = mine[off] * total.astype(BF16).astype(F32)
            routed = term if routed is None else routed + term
        squares[0] = jnp.sum(
            jnp.where(eye, jnp.sum(routed * routed, axis=1, keepdims=True), 0.0),
            axis=0,
            keepdims=True,
        )
        for ahead in range(chips - 1, 0, -1):
            for to_core in range(2):
                send(squares, ahead, squares_sem, lane_at(ahead, to_core))
        send(squares, 0, squares_sem, tp - 1)
        routed_v[0] = routed[:, :quarter]
        routed_v[1] = routed[:, quarter:]
        send(routed_v, 0, routed_sem, tp - 1)

    for copy in pairs:
        copy.wait_send()
    arrived(parts, parts_send)

    @pl.when(core == 0)
    def _():
        arrived(shares.at[pl.ds(0, chips)], share_send)
        arrived(resid_v.at[0], resid_sem.at[1])
        arrived(routed_v.at[0], routed_sem.at[1])
        arrived(squares.at[pl.ds(0, chips)], squares_sem.at[1])

    @pl.when(core == 1)
    def _():
        arrived(shares.at[pl.ds(0, chips - 1)], share_send)
        arrived(resid_v.at[0], resid_sem.at[0])
        arrived(routed_v.at[0], routed_sem.at[0])
        hidden = into_v.shape[3]
        arrived(into_v.at[0, 0, pl.ds(0, groups * seqs * width // hidden)], rows_send)
        arrived(squares.at[pl.ds(1, 2 * chips - 1)], squares_sem.at[0])
        arrived(squares.at[pl.ds(1, chips - 1)], squares_sem.at[1])

    total = squares[0]
    for other in range(1, chips):
        total = total + squares[other]
    scale = jnp.sum(
        jnp.where(eye, lax.rsqrt(total / width + EPS), 0.0), axis=1, keepdims=True
    )
    out_ref[...] = (
        resid_v[tp].astype(F32) + routed_v[core] * scale * heads_v[1]
    ).astype(BF16)


def per_device(*args):
    (
        tokens,
        memory,
        log_scale,
        mix_gain_in,
        w_query,
        w_key,
        w_value,
        w_igate,
        w_fgate,
        igate_bias,
        fgate_bias,
        head_gain,
        w_output,
        mix_gain_out,
        ffn_gain_in,
        routes,
        route_weights,
        expert_gate,
        expert_up,
        expert_down,
        ffn_gain_out,
    ) = args
    groups = lax.axis_size("ep")
    lanes = lax.axis_size("tp")
    seqs, width = tokens.shape
    local_experts, _, hidden = expert_gate.shape
    top = routes.shape[1]
    if (
        local_experts != 1
        or log_scale.shape[1] != 1
        or 2 * top < groups
        or groups & (groups - 1)
        or groups < 4
        or lanes % 2
        or lanes < 4
        or memory.shape[3] % memory.shape[2]
        or memory.shape[3] * lanes != width
        or groups * seqs > hidden
        or width % hidden
    ):
        return routed_device(*args)
    quarter = width // lanes
    key_dim, value_dim = memory.shape[2:]
    vmem = pl.BlockSpec(memory_space=pltpu.VMEM)
    hbm = pl.BlockSpec(memory_space=pl.ANY)
    dma = pltpu.SemaphoreType.DMA
    operands = (
        tokens,
        memory,
        log_scale.T,
        mix_gain_in.reshape(1, -1),
        w_query,
        w_key,
        w_value,
        w_igate.T,
        w_fgate.T,
        igate_bias.reshape(1, 1),
        fgate_bias.reshape(1, 1),
        head_gain.reshape(1, -1),
        w_output,
        mix_gain_out.reshape(1, -1),
        ffn_gain_in.reshape(1, -1),
        routes.T,
        route_weights.T,
        expert_gate,
        expert_up,
        expert_down,
        ffn_gain_out.reshape(1, -1),
    )
    held = (2, 3, 15, 16)
    return pl.pallas_call(
        functools.partial(layer_kernel, groups, lanes),
        out_shape=pltpu.VMEM((seqs, quarter), BF16),
        in_specs=[hbm for _ in operands],
        out_specs=vmem,
        scratch_shapes=[
            *[pltpu.VMEM(operands[i].shape, operands[i].dtype) for i in held],
            pltpu.VMEM((2, 1, width), BF16),
            pltpu.VMEM((2, 1, 1), F32),
            pltpu.VMEM((2, 1, width), F32),
            pltpu.VMEM((2, 1, quarter), F32),
            pltpu.VMEM((seqs, width), BF16),
            pltpu.VMEM((seqs, key_dim, value_dim), F32),
            pltpu.VMEM((width, 2 * key_dim + value_dim), BF16),
            pltpu.VMEM(w_output.shape, BF16),
            pltpu.VMEM((2, 2, width, hidden), BF16),
            pltpu.VMEM((2, hidden, width), BF16),
            pltpu.VMEM((3 * seqs, seqs * key_dim), BF16),
            pltpu.VMEM((key_dim, seqs * key_dim), F32),
            pltpu.VMEM((seqs, value_dim), F32),
            pltpu.VMEM((lanes, seqs, width), BF16),
            pltpu.VMEM((seqs, width), BF16),
            pltpu.VMEM((groups // 2, seqs, width), BF16),
            pltpu.VMEM((lanes, seqs, quarter), BF16),
            pltpu.VMEM((groups // 2, lanes // 2, seqs, 2 * quarter), BF16),
            pltpu.VMEM((groups * lanes // 2, seqs, 2 * quarter), BF16),
            pltpu.VMEM((2, seqs, quarter), F32),
            pltpu.VMEM((lanes, 1, 128), F32),
            dma((5,)),
            dma((3,)),
            dma((4,)),
            dma((2,)),
            dma((2,)),
            dma((2,)),
            pltpu.SemaphoreType.REGULAR,
            dma(()),
            dma(()),
            dma(()),
            dma((groups // 2,)),
            dma((2,)),
            dma(()),
            dma(()),
            dma((2,)),
            dma((2,)),
        ],
        compiler_params=pltpu.CompilerParams(
            collective_id=0,
            has_side_effects=True,
            vmem_limit_bytes=59 * 1024 * 1024,
        ),
        name="layer",
    )(*operands)


def solution(mesh):
    return jax.shard_map(
        per_device,
        mesh=mesh,
        in_specs=(
            P("ep", None),
            P("ep", "tp", None, None),
            P("ep", "tp"),
            P(),
            P(None, "tp"),
            P(None, "tp"),
            P(None, "tp"),
            P(None, "tp"),
            P(None, "tp"),
            P("tp"),
            P("tp"),
            P("tp"),
            P("tp", None),
            P(),
            P(),
            P("ep", None),
            P("ep", None),
            P("ep", None, "tp"),
            P("ep", None, "tp"),
            P("ep", "tp", None),
            P("tp"),
        ),
        out_specs=P("ep", "tp"),
        check_vma=False,
    )
```
